32 devices in a mesh: fs: 8 (over z, core), tp: 4 (over y, x).
Axes of the slice: x: 2, y: 2, z: 4, core: 2. Of those that a mesh axis runs over, the one named last changes fastest.
Arguments:
- gate_pre: bfloat16 [8192, 5632], P('fs', 'tp'), may hold values from -6 to 6
- up_pre: bfloat16 [8192, 5632], P('fs', 'tp'), may hold values from -6 to 6
- gate_taps: bfloat16 [3, 5632], replicated, may hold values from -3.5 to 3.5
- up_taps: bfloat16 [3, 5632], replicated, may hold values from -3.5 to 3.5
- down_proj: bfloat16 [5632, 2048], P('tp', 'fs'), may hold values from -0.078125 to 0.078125
- cotangent: bfloat16 [8192, 2048], P(('fs', 'tp')), may hold values from -6 to 6
Outputs:
- gate_grad: bfloat16 [8192, 5632], P('fs', 'tp')
- up_grad: bfloat16 [8192, 5632], P('fs', 'tp')
- down_grad: float32 [5632, 2048], P('tp', 'fs')
- row_norms: float32 [5632], P('tp')
- tap_grads: float32 [2, 3, 5632], replicated
The draws below stay inside these ranges and needn't reach their ends.
All inputs are finite; a program needn't handle non-finite values.
Results may differ from the reference program's by a relative error of at most 0.0042.
Values may be sent and summed in bfloat16 or wider, within the bound.
No kernel may reach another device: no remote copies, remote signals or barrier semaphores. Data moves between devices by JAX's collectives and lax.ppermute only.
A program may use at most 128 MiB of HBM per device.

```python
import math
import jax
import jax.numpy as jnp
from jax import lax

D = 2048
FF = 5632
TAPS = 3
TOKENS = 8192
N_TP = 4


def with_spikes(array, own_key, source, target, parts, factor):
    owner, partner = [(jnp.arange(array.shape[position]) // (array.shape[position] // parts)).reshape([-1 if axis == position else 1 for axis in range(array.ndim)]) for position in (source, target)]
    chosen = jax.random.permutation(own_key, parts)[partner]
    strong = (owner == chosen) | (owner == (partner + parts // 2) % parts)
    return jnp.where(strong, factor * array, array)


def steps_of(key, dims, cuts, low, high):
    loudness = 1.0
    for position, parts in cuts:
        heights = jax.random.uniform(jax.random.fold_in(jax.random.fold_in(key, 6), position), (parts,), jnp.float32, low / len(cuts), high / len(cuts))
        loudness = loudness * jnp.repeat(jnp.exp(heights), dims[position] // parts).reshape((-1,) + (1,) * (len(dims) - 1 - position))
    return loudness


def centred(own_key, extent, width, bound, shards=(), dtype=jnp.bfloat16):
    drawn = jax.random.normal(own_key, extent, jnp.float32) * width
    if len(shards) > 0:
        drawn = steps_of(own_key, extent, shards, -0.22, 0.18) * drawn
    return jnp.clip(drawn, min=-bound, max=bound).astype(dtype)


def bell_draw_with(rng, extent, deviation, most, cuts, heavy, held_as=jnp.bfloat16):
    array = deviation * jax.random.normal(rng, extent, jnp.float32)
    if cuts:
        array = array * steps_of(rng, extent, cuts, -0.22, 0.18)
    return jnp.clip(with_spikes(array, jax.random.fold_in(rng, 3), *heavy), -most, most).astype(held_as)


def setup_inputs(seed: int = 0) -> dict:
    key_of = jax.random.split(jax.random.key(seed), 7)
    gate_pre = centred(key_of[0], (TOKENS, FF), 1.0, 6.0, ((0, 8), (1, 4)))
    up_pre = centred(key_of[1], (TOKENS, FF), 1.0, 6.0, ((0, 8), (1, 4)))
    gate_taps = centred(key_of[2], (TAPS, FF), TAPS ** -0.5, 3.5)
    up_taps = centred(key_of[3], (TAPS, FF), TAPS ** -0.5, 3.5)
    down_proj = centred(key_of[4], (FF, D), FF ** -0.5, 0.078125, ((0, 4), (1, 8)))
    cotangent = bell_draw_with(key_of[5], (TOKENS, D), 1.0, 6.0, ((0, 32),), (0, 1, 32, 2.75))
    return dict(gate_pre=gate_pre, up_pre=up_pre, gate_taps=gate_taps, up_taps=up_taps, down_proj=down_proj, cotangent=cotangent)


def block_grads(gate_block, up_block, gate_tap_block, up_tap_block, down_block, cotangent):
    count = gate_block.shape[0]
    reach = TAPS - 1
    gate_taps_f = gate_tap_block.astype(jnp.float32)
    up_taps_f = up_tap_block.astype(jnp.float32)
    gate_padded = jnp.pad(gate_block.astype(jnp.float32), ((reach, 0), (0, 0)))
    up_padded = jnp.pad(up_block.astype(jnp.float32), ((reach, 0), (0, 0)))
    gate_conv = gate_taps_f[0] * gate_padded[0:count]
    up_conv = up_taps_f[0] * up_padded[0:count]
    for offset in range(1, TAPS):
        gate_conv = gate_conv + gate_taps_f[offset] * gate_padded[offset:offset + count]
        up_conv = up_conv + up_taps_f[offset] * up_padded[offset:offset + count]
    gate_sigmoid = jax.nn.sigmoid(gate_conv)
    gate_act = gate_conv * gate_sigmoid
    hidden = (gate_act * up_conv).astype(jnp.bfloat16)
    hidden_grad = jnp.dot(cotangent, down_block.T, preferred_element_type=jnp.float32)
    gate_conv_grad = hidden_grad * up_conv * gate_sigmoid * (1.0 + gate_conv * (1.0 - gate_sigmoid))
    up_conv_grad = hidden_grad * gate_act
    gate_grad_pad = jnp.pad(gate_conv_grad, ((0, reach), (0, 0)))
    up_grad_pad = jnp.pad(up_conv_grad, ((0, reach), (0, 0)))
    gate_grad = gate_taps_f[0] * gate_grad_pad[reach:reach + count]
    up_grad = up_taps_f[0] * up_grad_pad[reach:reach + count]
    for offset in range(1, TAPS):
        lead = reach - offset
        gate_grad = gate_grad + gate_taps_f[offset] * gate_grad_pad[lead:lead + count]
        up_grad = up_grad + up_taps_f[offset] * up_grad_pad[lead:lead + count]
    grad_scale = 1.0 / math.sqrt(TOKENS)
    gate_tap_terms = jnp.stack([lax.optimization_barrier(jnp.sum(gate_conv_grad * gate_padded[offset:offset + count], axis=0)) for offset in range(TAPS)])
    up_tap_terms = jnp.stack([lax.optimization_barrier(jnp.sum(up_conv_grad * up_padded[offset:offset + count], axis=0)) for offset in range(TAPS)])
    tap_terms = jnp.stack([gate_tap_terms, up_tap_terms]) * grad_scale
    down_term = jnp.dot(hidden.T, cotangent, preferred_element_type=jnp.float32) * grad_scale
    norms = lax.optimization_barrier(jnp.sum(down_term * down_term, axis=1)) / down_term.shape[1]
    return (gate_grad.astype(jnp.bfloat16), up_grad.astype(jnp.bfloat16), down_term, norms, tap_terms)

def reference(gate_pre, up_pre, gate_taps, up_taps, down_proj, cotangent):
    channels = FF // N_TP
    gate_blocks = gate_pre.reshape(TOKENS, N_TP, channels).transpose(1, 0, 2)
    up_blocks = up_pre.reshape(TOKENS, N_TP, channels).transpose(1, 0, 2)
    gate_tap_blocks = gate_taps.reshape(TAPS, N_TP, channels).transpose(1, 0, 2)
    up_tap_blocks = up_taps.reshape(TAPS, N_TP, channels).transpose(1, 0, 2)
    down_blocks = down_proj.reshape(N_TP, channels, D)
    gate_grad, up_grad, down_grad, row_norms, tap_grads = lax.map(lambda items: block_grads(items[0], items[1], items[2], items[3], items[4], cotangent), (gate_blocks, up_blocks, gate_tap_blocks, up_tap_blocks, down_blocks))
    gate_grad = gate_grad.transpose(1, 0, 2).reshape(TOKENS, FF)
    up_grad = up_grad.transpose(1, 0, 2).reshape(TOKENS, FF)
    down_grad = down_grad.reshape(FF, D)
    row_norms = row_norms.reshape(FF)
    tap_grads = tap_grads.transpose(1, 2, 0, 3).reshape(2, TAPS, FF)
    return (gate_grad, up_grad, down_grad, row_norms, tap_grads)
```

```python
import math

import jax
import jax.numpy as jnp
from jax import lax
from jax.experimental import pallas as pl
from jax.experimental.pallas import tpu as pltpu
from jax.sharding import PartitionSpec as P


def from_behind(block, axis, distance):
    devices = range(lax.axis_size(axis))
    route = [(i - distance, i) for i in devices if i - distance in devices]
    return lax.ppermute(block, axis, route)


def general_body(gate_pre, up_pre, gate_taps, up_taps, down_proj, cotangent):
    row_count = gate_pre.shape[0]
    channels = gate_pre.shape[1]
    tap_count = gate_taps.shape[0]
    reach = tap_count - 1
    channel_start = lax.axis_index("tp") * channels
    gate_taps_f = lax.dynamic_slice_in_dim(gate_taps, channel_start, channels, 1).astype(
        jnp.float32
    )
    up_taps_f = lax.dynamic_slice_in_dim(up_taps, channel_start, channels, 1).astype(jnp.float32)
    before = from_behind((gate_pre[row_count - reach :], up_pre[row_count - reach :]), "fs", 1)
    gate_padded = jnp.concatenate([before[0], gate_pre], axis=0).astype(jnp.float32)
    up_padded = jnp.concatenate([before[1], up_pre], axis=0).astype(jnp.float32)
    gate_conv = gate_taps_f[0] * gate_padded[0:row_count]
    up_conv = up_taps_f[0] * up_padded[0:row_count]
    for offset in range(1, tap_count):
        gate_conv = gate_conv + gate_taps_f[offset] * gate_padded[offset : offset + row_count]
        up_conv = up_conv + up_taps_f[offset] * up_padded[offset : offset + row_count]
    gate_sigmoid = jax.nn.sigmoid(gate_conv)
    gate_act = gate_conv * gate_sigmoid
    hidden = (gate_act * up_conv).astype(jnp.bfloat16)
    whole_cot = lax.all_gather(cotangent, "tp", axis=0, tiled=True)
    cot_cols = whole_cot
    hidden_grad = lax.dot_general(
        cot_cols,
        lax.all_gather(down_proj, "fs", axis=1, tiled=True),
        (((1,), (1,)), ((), ())),
        preferred_element_type=jnp.float32,
    )
    gate_conv_grad = hidden_grad * up_conv * gate_sigmoid * (1.0 + gate_conv * (1.0 - gate_sigmoid))
    up_conv_grad = hidden_grad * gate_act
    following = from_behind((gate_conv_grad[0:reach], up_conv_grad[0:reach]), "fs", -1)
    gate_grad_pad = jnp.concatenate([gate_conv_grad, following[0]], axis=0)
    up_grad_pad = jnp.concatenate([up_conv_grad, following[1]], axis=0)
    gate_grad = gate_taps_f[0] * gate_grad_pad[reach : reach + row_count]
    up_grad = up_taps_f[0] * up_grad_pad[reach : reach + row_count]
    for offset in range(1, tap_count):
        lead = reach - offset
        gate_grad = gate_grad + gate_taps_f[offset] * gate_grad_pad[lead : lead + row_count]
        up_grad = up_grad + up_taps_f[offset] * up_grad_pad[lead : lead + row_count]
    gate_tap_terms = jnp.stack(
        [
            jnp.sum(gate_conv_grad * gate_padded[offset : offset + row_count], axis=0)
            for offset in range(tap_count)
        ]
    )
    up_tap_terms = jnp.stack(
        [
            jnp.sum(up_conv_grad * up_padded[offset : offset + row_count], axis=0)
            for offset in range(tap_count)
        ]
    )
    tap_terms = jnp.stack([gate_tap_terms, up_tap_terms])
    feature_count = whole_cot.shape[1]
    grad_scale = 1.0 / math.sqrt(row_count * lax.axis_size("fs"))
    cot_cols = whole_cot
    own_rows = (
        lax.psum_scatter(
            lax.dot_general(
                cot_cols, hidden, (((0,), (0,)), ((), ())), preferred_element_type=jnp.float32
            ),
            "fs",
            scatter_dimension=0,
            tiled=True,
        )
        * grad_scale
    )
    down_grad = own_rows.T
    partial_norms = jnp.sum(own_rows * own_rows, axis=0)
    norm_sum, tap_sum = lax.psum((partial_norms, tap_terms), "fs")
    row_norms = norm_sum / feature_count
    tap_grads = lax.all_gather(tap_sum * grad_scale, "tp", axis=2, tiled=True)
    return (
        gate_grad.astype(jnp.bfloat16),
        up_grad.astype(jnp.bfloat16),
        down_grad,
        row_norms,
        tap_grads,
    )


def line_pairs(chips, step, first, last):
    return [
        (2 * chip + core, 2 * (chip + step) + core)
        for chip in range(first, last + 1)
        for core in range(2)
        if 0 <= chip + step < chips
    ]


def gather_rows(block):
    rows = block.shape[0]
    half = rows // 2
    me = lax.axis_index("tp")
    x_route = [(i, i ^ 1) for i in range(4)]
    y_route = [(i, i ^ 2) for i in range(4)]
    from_x = lax.ppermute(block, "tp", x_route)
    from_y = lax.ppermute(block, "tp", y_route)
    diag_top = lax.ppermute(from_x[:half], "tp", y_route)
    diag_low = lax.ppermute(from_y[half:], "tp", x_route)
    whole = jnp.zeros((4 * rows, block.shape[1]), block.dtype)
    for piece, start in (
        (block, me * rows),
        (from_x, (me ^ 1) * rows),
        (from_y, (me ^ 2) * rows),
        (diag_top, (me ^ 3) * rows),
        (diag_low, (me ^ 3) * rows + half),
    ):
        whole = lax.dynamic_update_slice_in_dim(whole, piece, start, 0)
    return whole


def swap_cores(block):
    return lax.ppermute(block, "fs", [(i, i ^ 1) for i in range(8)])


def after(values, earlier):
    return lax.optimization_barrier((values, earlier))[0]


def line_shards(own):
    ups = [own]
    downs = [own]
    for step in range(1, 4):
        ups.append(lax.ppermute(ups[-1], "fs", line_pairs(4, 1, step - 1, 3)))
        downs.append(lax.ppermute(downs[-1], "fs", line_pairs(4, -1, 0, 4 - step)))
    return ups, downs


def in_order(own, ups, downs, chip):
    shards = []
    for source in (0, 3, 1, 2):
        shard = own
        for at in range(4):
            if at > source:
                shard = jnp.where(chip == at, ups[at - source], shard)
            elif at < source:
                shard = jnp.where(chip == at, downs[source - at], shard)
        shards.append(shard)
    return jnp.concatenate(shards, axis=1)


LANES = 128
STEP = 32


def grads_kernel(
    grad, gate, up, gate_prev, up_prev, before, carry, taps, *rest, start, total, rows
):
    gate_out, up_out, sums, edge, xg, xu, gs, us, held = rest[-9:]
    step = pl.program_id(0)
    block = start - step

    @pl.when(step == 0)
    def _():
        held[...] = carry[...]
        sums[...] = jnp.zeros_like(sums)

    def column(index, unused):
        lanes = pl.ds(pl.multiple_of(index * LANES, LANES), LANES)
        first = block == 0
        xg[0:8] = jnp.where(first, before[0:8, lanes], gate_prev[:, lanes].astype(jnp.float32)[8:])
        xu[0:8] = jnp.where(first, before[8:16, lanes], up_prev[:, lanes].astype(jnp.float32)[8:])
        xg[8:] = gate[:, lanes].astype(jnp.float32)
        xu[8:] = up[:, lanes].astype(jnp.float32)
        gs[rows:] = held[0:8, lanes]
        us[rows:] = held[8:16, lanes]
        tg = [taps[k : k + 1, lanes] for k in range(3)]
        tu = [taps[k + 3 : k + 4, lanes] for k in range(3)]
        acc = [jnp.zeros((8, LANES), jnp.float32) for _ in range(6)]
        for at in range(0, rows, STEP):
            pg = [xg[pl.ds(at + 6 + k, STEP)] for k in range(3)]
            pu = [xu[pl.ds(at + 6 + k, STEP)] for k in range(3)]
            conv = tg[0] * pg[0] + tg[1] * pg[1] + tg[2] * pg[2]
            up_conv = tu[0] * pu[0] + tu[1] * pu[1] + tu[2] * pu[2]
            sig = jax.nn.sigmoid(conv)
            h = grad[pl.ds(at, STEP), lanes]
            dg = h * up_conv * sig * (1.0 + conv * (1.0 - sig))
            du = h * (conv * sig)
            gs[pl.ds(at, STEP)] = dg
            us[pl.ds(at, STEP)] = du
            for k in range(3):
                acc[k] += jnp.sum((dg * pg[k]).reshape(STEP // 8, 8, LANES), axis=0)
                acc[k + 3] += jnp.sum((du * pu[k]).reshape(STEP // 8, 8, LANES), axis=0)
        for k in range(6):
            sums[k : k + 1, lanes] += jnp.sum(acc[k], axis=0, keepdims=True)
        for at in range(0, rows, STEP):
            for out, source, tap in ((gate_out, gs, tg), (up_out, us, tu)):
                value = tap[0] * source[pl.ds(at + 2, STEP)]
                value = value + tap[1] * source[pl.ds(at + 1, STEP)]
                value = value + tap[2] * source[pl.ds(at, STEP)]
                out[pl.ds(at, STEP), lanes] = value.astype(jnp.bfloat16)
        held[0:8, lanes] = gs[0:8]
        held[8:16, lanes] = us[0:8]
        return unused

    lax.fori_loop(0, grad.shape[1] // LANES, column, 0)
    edge[...] = held[...]


def grads_part(grad, gate, up, before, carry, taps, start, count, rows, filled=()):
    total, channels = gate.shape
    main = pl.BlockSpec((rows, channels), lambda i: (start - i, 0))
    local = pl.BlockSpec((rows, channels), lambda i: (count - 1 - i, 0))
    prev = pl.BlockSpec(
        (16, channels), lambda i: (jnp.maximum((start - i) * (rows // 16) - 1, 0), 0)
    )
    whole = lambda n: pl.BlockSpec((n, channels), lambda i: (0, 0))
    return pl.pallas_call(
        lambda *refs: grads_kernel(*refs, start=start, total=total, rows=rows),
        grid=(count,),
        in_specs=[local, main, main, prev, prev, whole(16), whole(16), whole(8)]
        + [pl.BlockSpec(memory_space=pl.ANY)] * len(filled),
        out_specs=[main, main, whole(8), whole(16)],
        out_shape=[
            jax.ShapeDtypeStruct(gate.shape, jnp.bfloat16),
            jax.ShapeDtypeStruct(gate.shape, jnp.bfloat16),
            jax.ShapeDtypeStruct((8, channels), jnp.float32),
            jax.ShapeDtypeStruct((16, channels), jnp.float32),
        ],
        scratch_shapes=[pltpu.VMEM((rows + 8, LANES), jnp.float32)] * 4
        + [pltpu.VMEM((16, channels), jnp.float32)],
        input_output_aliases={8 + i: i for i in range(len(filled))},
    )(grad, gate, up, gate, up, before, carry, taps, *filled)


def plus(piece, received):
    return (piece + received.astype(jnp.float32)).astype(jnp.bfloat16)


def first_sends(p, chip):
    up = lax.ppermute(p[3].astype(jnp.bfloat16), "fs", line_pairs(4, 1, 0, 0))
    down = lax.ppermute(p[0].astype(jnp.bfloat16), "fs", line_pairs(4, -1, 3, 3))
    return up, down


def second_pieces(p, chip, up, down):
    up_send = plus(jnp.where(chip == 0, p[2], p[3]), up)
    down_send = plus(jnp.where(chip == 3, p[1], p[0]), down)
    return up_send, down_send


def third_pieces(p, chip, up, down):
    up_send = plus(jnp.where(chip == 0, p[1], jnp.where(chip == 1, p[2], p[3])), up)
    down_send = plus(jnp.where(chip == 3, p[2], jnp.where(chip == 2, p[1], p[0])), down)
    return up_send, down_send


def send_both(up_send, down_send, step):
    up = lax.ppermute(up_send, "fs", line_pairs(4, 1, 0, step - 1))
    down = lax.ppermute(down_send, "fs", line_pairs(4, -1, 4 - step, 3))
    return up, down


def line_body(gate_pre, up_pre, gate_taps, up_taps, down_proj, cotangent):
    row_count, channels = gate_pre.shape
    tap_count = gate_taps.shape[0]
    reach = tap_count - 1
    place = lax.axis_index("fs")
    chip = place // 2
    core = place % 2
    width = down_proj.shape[1]
    feature_count = cotangent.shape[1]
    grad_scale = 1.0 / math.sqrt(row_count * lax.axis_size("fs"))

    split = cotangent.reshape(cotangent.shape[0], 4, 2, width)
    mine = lax.dynamic_index_in_dim(split, core, 2, keepdims=False)
    other = lax.dynamic_index_in_dim(split, 1 - core, 2, keepdims=False)

    def chunk(first, second):
        return jnp.concatenate(
            [mine[:, first], mine[:, second], other[:, first], other[:, second]], axis=1
        )

    cot_outer = gather_rows(chunk(0, 3))
    cot_inner = gather_rows(chunk(1, 2))

    before = from_behind(
        jnp.concatenate([gate_pre[row_count - reach :], up_pre[row_count - reach :]], axis=0),
        "fs",
        1,
    )
    channel_start = lax.axis_index("tp") * channels
    gate_taps_f = lax.dynamic_slice_in_dim(gate_taps, channel_start, channels, 1).astype(
        jnp.float32
    )
    up_taps_f = lax.dynamic_slice_in_dim(up_taps, channel_start, channels, 1).astype(jnp.float32)
    ups, downs = line_shards(down_proj)

    gate_padded = jnp.concatenate([before[:reach], gate_pre], axis=0).astype(jnp.float32)
    up_padded = jnp.concatenate([before[reach:], up_pre], axis=0).astype(jnp.float32)
    gate_conv = gate_taps_f[0] * gate_padded[0:row_count]
    up_conv = up_taps_f[0] * up_padded[0:row_count]
    for offset in range(1, tap_count):
        gate_conv = gate_conv + gate_taps_f[offset] * gate_padded[offset : offset + row_count]
        up_conv = up_conv + up_taps_f[offset] * up_padded[offset : offset + row_count]
    gate_sigmoid = jax.nn.sigmoid(gate_conv)
    gate_act = gate_conv * gate_sigmoid
    hidden = (gate_act * up_conv).astype(jnp.bfloat16)

    hidden_peer = swap_cores(hidden)
    contract_rows = (((0,), (0,)), ((), ()))

    def pieces(cot):
        peer = swap_cores(cot[:, 2 * width :])
        out = lax.dot_general(
            cot[:, : 2 * width], hidden, contract_rows, preferred_element_type=jnp.float32
        ) + lax.dot_general(peer, hidden_peer, contract_rows, preferred_element_type=jnp.float32)
        return out[:width], out[width:]

    p0, p3 = pieces(cot_outer)
    p1, p2 = pieces(cot_inner)
    p = [p0, p1, p2, p3]
    up, down = first_sends(p, chip)

    cot_all = jnp.concatenate(
        [block[:, side * width : (side + 2) * width] for side in (0, 2) for block in (cot_outer, cot_inner)],
        axis=1,
    )
    ups[3], downs[3] = after((ups[3], downs[3]), (p1, p2))
    proj_mine = in_order(down_proj, ups, downs, chip)
    proj_other = swap_cores(proj_mine)
    proj_all = jnp.concatenate([proj_mine, proj_other], axis=1)
    contract_features = (((1,), (1,)), ((), ()))
    rows = row_count // 4
    low_grad = lax.dot_general(
        cot_all[: 2 * rows], proj_all, contract_features, preferred_element_type=jnp.float32
    )
    high_grad = lax.dot_general(
        cot_all[2 * rows :], proj_all, contract_features, preferred_element_type=jnp.float32
    )
    head_grad = low_grad[:reach]
    head_conv = sum(gate_taps_f[k] * gate_padded[k : k + reach] for k in range(tap_count))
    head_up = sum(up_taps_f[k] * up_padded[k : k + reach] for k in range(tap_count))
    head_sig = jax.nn.sigmoid(head_conv)
    spare = jnp.zeros((8 - reach, channels), jnp.float32)
    head = jnp.concatenate(
        [
            head_grad * head_up * head_sig * (1.0 + head_conv * (1.0 - head_sig)),
            head_grad * (head_conv * head_sig),
        ]
    )
    following = from_behind(head, "fs", -1)
    carry = jnp.concatenate([following[:reach], spare, following[reach:], spare])
    before_f = before.astype(jnp.float32)
    ahead = jnp.concatenate([spare, before_f[:reach], spare, before_f[reach:]])
    taps = jnp.concatenate([gate_taps_f, up_taps_f, jnp.zeros((2, channels), jnp.float32)])

    up, down = lax.optimization_barrier((up, down))
    up_send, down_send = second_pieces(p, chip, up, down)
    up, down = send_both(up_send, down_send, 2)
    up, down = after((up, down), (high_grad, low_grad))
    up_send, down_send = third_pieces(p, chip, up, down)
    up, down = send_both(up_send, down_send, 3)
    high_grad, low_grad = after((high_grad, low_grad), (up_send, down_send))
    gate_high, up_high, sums_high, edge = grads_part(
        high_grad, gate_pre, up_pre, ahead, carry, taps, 3, 2, rows
    )
    gate_grad, up_grad, sums_low, _ = grads_part(
        low_grad, gate_pre, up_pre, ahead, edge, taps, 1, 2, rows, (gate_high, up_high)
    )
    tap_terms = (sums_high + sums_low)[: 2 * tap_count]
    own = jnp.where(chip < 2, jnp.where(chip == 0, p[0], p[1]), jnp.where(chip == 2, p[2], p[3]))
    own_rows = (own + up.astype(jnp.float32) + down.astype(jnp.float32)) * grad_scale
    partial_norms = jnp.sum(own_rows * own_rows, axis=0)
    stacked = jnp.concatenate([tap_terms, partial_norms[None]])
    sums = jnp.sum(lax.all_gather(stacked, "fs", axis=0), axis=0)
    row_norms = sums[2 * tap_count] / feature_count
    tap_sum = sums[: 2 * tap_count].reshape(2, tap_count, channels) * grad_scale
    tap_grads = lax.all_gather(tap_sum, "tp", axis=2, tiled=True)
    return gate_grad, up_grad, own_rows.T, row_norms, tap_grads


def body(*args):
    if lax.axis_size("fs") == 8 and lax.axis_size("tp") == 4:
        return line_body(*args)
    return general_body(*args)


def solution(mesh):
    placed = (P("fs", "tp"), P("fs", "tp"), P(), P(), P("tp", "fs"), P(("fs", "tp"), None))
    return jax.shard_map(
        body,
        mesh=mesh,
        in_specs=placed,
        out_specs=(P("fs", "tp"), P("fs", "tp"), P("tp", "fs"), P("tp"), P()),
        check_vma=False,
    )
```
